32 devices in a mesh: fs: 16 (over z, y, x), tp: 2 (over core).
Axes of the slice: x: 2, y: 2, z: 4, core: 2. Of those that a mesh axis runs over, the one named last changes fastest.
Arguments:
- tokens: bfloat16 [4096, 2048], P('fs', 'tp'), may hold values from -6 to 6
- mixer_norm_gain: bfloat16 [2048], replicated, may hold values from 0.099609375 to 1.8984375
- recurrence_branch_weight: bfloat16 [2048, 1024], P('fs', 'tp'), may hold values from -0.125 to 0.125
- output_gate_projection: bfloat16 [2048, 1024], P('fs', 'tp'), may hold values from -0.125 to 0.125
- recurrence_conv_taps: bfloat16 [4, 1024], P(None, 'tp'), may hold values from -3 to 3
- recurrence_gate_map: bfloat16 [16, 64, 64], P('tp'), may hold values from -0.75 to 0.75
- input_gate_map: bfloat16 [16, 64, 64], P('tp'), may hold values from -0.75 to 0.75
- channel_decay_rate: float32 [1024], P('tp'), may hold values from 0.001 to 0.03
- position_log_decay: float32 [4096, 1024], P('fs', 'tp'), may hold values from -0.69 to 0
- mixer_output_weight: bfloat16 [1024, 2048], P('tp', 'fs'), may hold values from -0.75 to 0.75
- feedforward_norm_gain: bfloat16 [2048], replicated, may hold values from 0.099609375 to 1.8984375
- gate_up_weight: bfloat16 [2048, 5632], P('fs', 'tp'), may hold values from -0.125 to 0.125
- value_up_weight: bfloat16 [2048, 5632], P('fs', 'tp'), may hold values from -0.125 to 0.125
- gate_conv_taps: bfloat16 [3, 5632], P(None, 'tp'), may hold values from -3 to 3
- value_conv_taps: bfloat16 [3, 5632], P(None, 'tp'), may hold values from -3 to 3
- down_projection_weight: bfloat16 [5632, 2048], P('tp', 'fs'), may hold values from -0.15625 to 0.15625
Outputs:
- result: bfloat16 [4096, 2048], P('fs', 'tp')
The draws below stay inside these ranges and needn't reach their ends.
All inputs are finite; a program needn't handle non-finite values.
Results may differ from the reference program's by a relative error of at most 0.024.
Values may be sent and summed in bfloat16 or wider, within the bound.
A program may use at most 128 MiB of HBM per device.

```python
import math
import jax
import jax.numpy as jnp
from jax import lax

D = 2048
HEADS = 16
HEAD_DIM = 64
W = 1024
FF = 5632
SEQ_LEN = 64
TOKENS = 4096
N_TP = 2


def draw_channel_decay_rate(key, part):
    base = jax.random.fold_in(key, 17)
    key_pick, key_slow, key_fast = jax.random.split(base, 3)
    limit = 5
    picked = jax.random.randint(key_pick, (W,), 0, 10) < limit
    slow_rate = jnp.exp(jax.random.uniform(key_slow, (W,), jnp.float32, math.log(0.001), math.log(0.004)))
    fast_rate = jnp.exp(jax.random.uniform(key_fast, (W,), jnp.float32, math.log(0.012), math.log(0.03)))
    return jnp.where(picked, slow_rate, fast_rate).astype(jnp.float32)


def draw_position_log_decay(key, part):
    base = jax.random.fold_in(key, 29)
    key_marks, key_depth = jax.random.split(base, 2)
    marks = (jax.random.randint(key_marks, (TOKENS, 1), 0, 32) == 0).astype(jnp.float32)
    depth = jax.random.uniform(key_depth, (TOKENS, W), jnp.float32, 0.22, 0.69)
    return (-marks * depth).astype(jnp.float32)


def steps_of(rng, extent, pieces, low, top_value):
    level, own = 1.0, jax.random.fold_in(rng, 6)
    for position, parts in pieces:
        steps = jnp.exp(jax.random.uniform(jax.random.fold_in(own, position), (parts,), jnp.float32, low / len(pieces), top_value / len(pieces)))
        level = level * jnp.repeat(steps, extent[position] // parts).reshape([-1 if axis == position else 1 for axis in range(len(extent))])
    return level


def normal_values(stream_key, extent, scale, most, shards=(), dtype=jnp.bfloat16):
    drawn = jax.random.normal(stream_key, extent, jnp.float32) * scale
    if len(shards) > 0:
        drawn = steps_of(stream_key, extent, shards, -0.22, 0.18) * drawn
    return jnp.clip(drawn, min=-most, max=most).astype(dtype)


def setup_inputs(seed: int = 0) -> dict:
    key_list = jax.random.split(jax.random.key(seed), 17)
    tokens = normal_values(key_list[0], (TOKENS, D), 1.0, 6.0, ((0, 16), (1, 2)))
    mixer_norm_gain = jnp.clip(1.0 + 0.18 * jax.random.normal(key_list[1], (D,), jnp.float32), 0.099609375, 1.8984375).astype(jnp.bfloat16)
    recurrence_branch_weight = normal_values(key_list[2], (D, W), D ** -0.5, 0.125, ((0, 16), (1, 2)))
    output_gate_projection = normal_values(key_list[3], (D, W), D ** -0.5, 0.125, ((0, 16), (1, 2)))
    recurrence_conv_taps = normal_values(key_list[4], (4, W), 0.5, 3.0, ((1, 2),))
    recurrence_gate_map = normal_values(key_list[5], (HEADS, HEAD_DIM, HEAD_DIM), HEAD_DIM ** -0.5, 0.75, ((0, 2),))
    input_gate_map = normal_values(key_list[6], (HEADS, HEAD_DIM, HEAD_DIM), HEAD_DIM ** -0.5, 0.75, ((0, 2),))
    channel_decay_rate = draw_channel_decay_rate(jax.random.fold_in(key_list[16], 71), 0)
    position_log_decay = draw_position_log_decay(jax.random.fold_in(key_list[16], 71), 0)
    mixer_output_weight = normal_values(key_list[9], (W, D), (W // 16) ** -0.5, 0.75, ((0, 2), (1, 16)))
    feedforward_norm_gain = jnp.clip(1.0 + 0.18 * jax.random.normal(key_list[10], (D,), jnp.float32), 0.099609375, 1.8984375).astype(jnp.bfloat16)
    gate_up_weight = normal_values(key_list[11], (D, FF), D ** -0.5, 0.125, ((0, 16), (1, 2)))
    value_up_weight = normal_values(key_list[12], (D, FF), D ** -0.5, 0.125, ((0, 16), (1, 2)))
    gate_conv_taps = normal_values(key_list[13], (3, FF), 0.6, 3.0, ((1, 2),))
    value_conv_taps = normal_values(key_list[14], (3, FF), 0.6, 3.0, ((1, 2),))
    down_projection_weight = normal_values(key_list[15], (FF, D), (FF // 4) ** -0.5, 0.15625, ((0, 2), (1, 16)))
    return {"tokens": tokens, "mixer_norm_gain": mixer_norm_gain, "recurrence_branch_weight": recurrence_branch_weight, "output_gate_projection": output_gate_projection, "recurrence_conv_taps": recurrence_conv_taps, "recurrence_gate_map": recurrence_gate_map, "input_gate_map": input_gate_map, "channel_decay_rate": channel_decay_rate, "position_log_decay": position_log_decay, "mixer_output_weight": mixer_output_weight, "feedforward_norm_gain": feedforward_norm_gain, "gate_up_weight": gate_up_weight, "value_up_weight": value_up_weight, "gate_conv_taps": gate_conv_taps, "value_conv_taps": value_conv_taps, "down_projection_weight": down_projection_weight}


EPS = 1e-06
DECAY_RATE_GAIN = 8.0

def rms_normed(values, gain):
    wide = values.astype(jnp.float32)
    factor = lax.rsqrt(lax.optimization_barrier(jnp.mean(wide * wide, axis=-1, keepdims=True)) + EPS)
    return (wide * factor * gain.astype(jnp.float32)).astype(jnp.bfloat16)

def causal_conv(values, kernel):
    width = kernel.shape[0]
    row_count, channels = values.shape
    grouped = values.astype(jnp.float32).reshape(row_count // SEQ_LEN, SEQ_LEN, channels)
    padded = jnp.pad(grouped, ((0, 0), (width - 1, 0), (0, 0)))
    summed = padded[:, 0:SEQ_LEN] * kernel[0].astype(jnp.float32)
    for offset in range(1, width):
        summed = summed + padded[:, offset:offset + SEQ_LEN] * kernel[offset].astype(jnp.float32)
    return summed.reshape(row_count, channels)

def combine(left, right):
    first_a, first_b = left
    second_a, second_b = right
    return (first_a * second_a, second_a * first_b + second_b)

def block_sums(left, weight, blocks):
    width = left.shape[1] // blocks
    summed = jnp.zeros((left.shape[0], weight.shape[1]), jnp.float32)
    for index in range(blocks):
        partial_sum = jnp.dot(left[:, index * width:(index + 1) * width], weight[index * width:(index + 1) * width], preferred_element_type=jnp.float32)
        summed = summed + partial_sum.astype(jnp.bfloat16).astype(jnp.float32)
    return summed

def reference(tokens, mixer_norm_gain, recurrence_branch_weight, output_gate_projection, recurrence_conv_taps, recurrence_gate_map, input_gate_map, channel_decay_rate, position_log_decay, mixer_output_weight, feedforward_norm_gain, gate_up_weight, value_up_weight, gate_conv_taps, value_conv_taps, down_projection_weight):
    row_count = tokens.shape[0]
    normed = rms_normed(tokens, mixer_norm_gain)
    branch = jnp.dot(normed, recurrence_branch_weight, preferred_element_type=jnp.float32).astype(jnp.bfloat16)
    outgate = jnp.dot(normed, output_gate_projection, preferred_element_type=jnp.float32).astype(jnp.bfloat16)
    conv = causal_conv(branch, recurrence_conv_taps).astype(jnp.bfloat16)
    grouped = conv.astype(jnp.float32).reshape(row_count, HEADS, HEAD_DIM)
    recurrence_scan = jax.nn.sigmoid(jnp.einsum('rhi,hij->rhj', grouped, recurrence_gate_map.astype(jnp.float32)).reshape(row_count, W))
    inner = jax.nn.sigmoid(jnp.einsum('rhi,hij->rhj', grouped, input_gate_map.astype(jnp.float32)).reshape(row_count, W))
    log_alpha = -DECAY_RATE_GAIN * recurrence_scan * channel_decay_rate[None, :] + position_log_decay
    drive = jnp.sqrt(-jnp.expm1(2.0 * log_alpha)) * inner * conv.astype(jnp.float32)
    shape3 = (row_count // SEQ_LEN, SEQ_LEN, W)
    unused, state = lax.associative_scan(combine, (jnp.exp(log_alpha).reshape(shape3), drive.reshape(shape3)), axis=1)
    state = state.reshape(row_count, W)
    mixed = (state * jax.nn.gelu(outgate.astype(jnp.float32))).astype(jnp.bfloat16)
    after = (tokens.astype(jnp.float32) + block_sums(mixed, mixer_output_weight, N_TP)).astype(jnp.bfloat16)
    normed2 = rms_normed(after, feedforward_norm_gain)
    gate_half = jnp.dot(normed2, gate_up_weight, preferred_element_type=jnp.float32).astype(jnp.bfloat16)
    value_half = jnp.dot(normed2, value_up_weight, preferred_element_type=jnp.float32).astype(jnp.bfloat16)
    hidden = (jax.nn.silu(causal_conv(gate_half, gate_conv_taps)) * causal_conv(value_half, value_conv_taps)).astype(jnp.bfloat16)
    return (after.astype(jnp.float32) + block_sums(hidden, down_projection_weight, N_TP)).astype(jnp.bfloat16)
```

```python
import functools

import jax
import jax.numpy as jnp
from jax import lax
from jax.experimental import pallas as pl
from jax.experimental.pallas import tpu as pltpu
from jax.sharding import PartitionSpec as P

SEQ_LEN = 64


EPS = 1e-06
DECAY_RATE_GAIN = 8.0


def rms_normed(values, gain):
    wide = values.astype(jnp.float32)
    factor = lax.rsqrt(jnp.mean(wide * wide, axis=-1, keepdims=True) + EPS)
    return (wide * factor * gain.astype(jnp.float32)).astype(jnp.bfloat16)


def causal_conv(values, kernel):
    width = kernel.shape[0]
    row_count, channels = values.shape
    grouped = values.astype(jnp.float32).reshape(row_count // SEQ_LEN, SEQ_LEN, channels)
    padded = jnp.pad(grouped, ((0, 0), (width - 1, 0), (0, 0)))
    summed = padded[:, 0:SEQ_LEN] * kernel[0].astype(jnp.float32)
    for offset in range(1, width):
        summed = summed + padded[:, offset : offset + SEQ_LEN] * kernel[offset].astype(jnp.float32)
    return summed.reshape(row_count, channels)


def combine(left, right):
    first_a, first_b = left
    second_a, second_b = right
    return (first_a * second_a, second_a * first_b + second_b)


def pair_folder(normed, pieces):
    return (
        jnp.dot(normed, pieces[0], preferred_element_type=jnp.float32),
        jnp.dot(normed, pieces[1], preferred_element_type=jnp.float32),
    )


def gathered_layer(
    tokens,
    mixer_norm_gain,
    recurrence_branch_weight,
    output_gate_projection,
    recurrence_conv_taps,
    recurrence_gate_map,
    input_gate_map,
    channel_decay_rate,
    position_log_decay,
    mixer_output_weight,
    feedforward_norm_gain,
    gate_up_weight,
    value_up_weight,
    gate_conv_taps,
    value_conv_taps,
    down_projection_weight,
):
    row_count = tokens.shape[0]
    local_width = recurrence_branch_weight.shape[1]
    local_heads = recurrence_gate_map.shape[0]
    head_size = recurrence_gate_map.shape[1]
    whole_rows = lax.all_gather(tokens, "tp", axis=1, tiled=True)
    normed = rms_normed(whole_rows, mixer_norm_gain)
    branch_sum, outgate_sum = pair_folder(
        normed,
        (
            lax.all_gather(recurrence_branch_weight, "fs", axis=0, tiled=True),
            lax.all_gather(output_gate_projection, "fs", axis=0, tiled=True),
        ),
    )
    branch = branch_sum.astype(jnp.bfloat16)
    outgate = outgate_sum.astype(jnp.bfloat16)
    conv = causal_conv(branch, recurrence_conv_taps).astype(jnp.bfloat16)
    grouped = conv.reshape(row_count, local_heads, head_size)
    recurrence_scan = jax.nn.sigmoid(
        jnp.einsum(
            "rhi,hij->rhj", grouped, recurrence_gate_map, preferred_element_type=jnp.float32
        ).reshape(row_count, local_width)
    )
    inner = jax.nn.sigmoid(
        jnp.einsum(
            "rhi,hij->rhj", grouped, input_gate_map, preferred_element_type=jnp.float32
        ).reshape(row_count, local_width)
    )
    log_alpha = (
        -DECAY_RATE_GAIN * recurrence_scan * channel_decay_rate[None, :] + position_log_decay
    )
    drive = jnp.sqrt(-jnp.expm1(2.0 * log_alpha)) * inner * conv.astype(jnp.float32)
    shape3 = (row_count // SEQ_LEN, SEQ_LEN, local_width)
    unused, state = lax.associative_scan(
        combine, (jnp.exp(log_alpha).reshape(shape3), drive.reshape(shape3)), axis=1
    )
    state = state.reshape(row_count, local_width)
    mixed = (state * jax.nn.gelu(outgate.astype(jnp.float32))).astype(jnp.bfloat16)
    mixer_terms = jnp.dot(
        mixed,
        lax.all_gather(mixer_output_weight, "fs", axis=1, tiled=True),
        preferred_element_type=jnp.float32,
    )
    mixer_terms = mixer_terms.astype(jnp.bfloat16).astype(jnp.float32)
    mixer_whole = lax.psum(mixer_terms.astype(jnp.bfloat16), "tp").astype(jnp.float32)
    whole_after = (whole_rows.astype(jnp.float32) + mixer_whole).astype(jnp.bfloat16)
    normed2 = rms_normed(whole_after, feedforward_norm_gain)
    gate_whole, value_whole = (
        lax.all_gather(gate_up_weight, "fs", axis=0, tiled=True),
        lax.all_gather(value_up_weight, "fs", axis=0, tiled=True),
    )
    gate_sum = jnp.dot(normed2, gate_whole, preferred_element_type=jnp.float32)
    value_sum = jnp.dot(normed2, value_whole, preferred_element_type=jnp.float32)
    gate_half = gate_sum.astype(jnp.bfloat16)
    value_half = value_sum.astype(jnp.bfloat16)
    hidden = (
        jax.nn.silu(causal_conv(gate_half, gate_conv_taps))
        * causal_conv(value_half, value_conv_taps)
    ).astype(jnp.bfloat16)
    channel_terms = jnp.dot(
        hidden,
        lax.all_gather(down_projection_weight, "fs", axis=1, tiled=True),
        preferred_element_type=jnp.float32,
    )
    channel_terms = channel_terms.astype(jnp.bfloat16).astype(jnp.float32)
    channel_share = lax.psum_scatter(
        channel_terms.astype(jnp.bfloat16), "tp", scatter_dimension=1, tiled=True
    ).astype(jnp.float32)
    share_width = channel_share.shape[1]
    residual_share = lax.dynamic_slice_in_dim(
        whole_after, lax.axis_index("tp") * share_width, share_width, 1
    )
    return (residual_share.astype(jnp.float32) + channel_share).astype(jnp.bfloat16)


PLANE = 4
ANY = pl.BlockSpec(memory_space=pl.ANY)


def hop(src, dst, send, recv, target):
    return pltpu.make_async_remote_copy(
        src_ref=src,
        dst_ref=dst,
        send_sem=send,
        recv_sem=recv,
        device_id=target,
        device_id_type=pl.DeviceIdType.MESH,
    )


def greet(targets):
    barrier = pltpu.get_barrier_semaphore()
    for target in targets:
        pl.semaphore_signal(
            barrier, inc=1, device_id=target, device_id_type=pl.DeviceIdType.MESH
        )
    pl.semaphore_wait(barrier, len(targets))


def span(index, size):
    return pl.ds(pl.multiple_of(index * size, size), size)


def where_am_i(layers):
    fs, tp = lax.axis_index("fs"), lax.axis_index("tp")
    return fs, fs // PLANE, fs % PLANE, tp


def line_targets(layers, z, p, tp):
    return [(((z + s) % layers) * PLANE + p, tp) for s in range(1, layers)]


def weights_kernel(
    layers, tok, bo, mo, gu, dn, whole_tok, bo_all, mo_all, gu_all, dn_all, send, recv, tok_sems, local
):
    fs, z, p, tp = where_am_i(layers)
    y, x = p // 2, p % 2
    px, py = y * 2 + (x + 1) % 2, ((y + 1) % 2) * 2 + x
    pd = ((y + 1) % 2) * 2 + (x + 1) % 2
    x_target, y_target = (z * PLANE + px, tp), (z * PLANE + py, tp)
    core_target = (fs, 1 - tp)
    on_line = line_targets(layers, z, p, tp)
    greet(on_line + [x_target, y_target, core_target])

    half = tok.shape[1]
    deep = bo.shape[0]
    wide = mo.shape[1]

    def bo_at(f, part=None):
        if part is None:
            return bo_all.at[span(f, deep), :]
        return bo_all.at[span(f * 2 + part, deep // 2), :]

    def gu_at(f, part=None):
        if part is None:
            return gu_all.at[span(f, deep), :]
        return gu_all.at[span(f * 2 + part, deep // 2), :]

    def mo_at(f, part=None):
        rows = mo.shape[0]
        if part is None:
            return mo_all.at[:, span(f, wide)]
        return mo_all.at[pl.ds(part * (rows // 2), rows // 2), span(f, wide)]

    def dn_at(f, part=None):
        rows = dn.shape[1]
        if part is None:
            return dn_all.at[:, span(f, wide)]
        return dn_all.at[pl.ds(part * (rows // 2), rows // 2), span(f, wide)]

    arrays = (
        (bo_at, lambda zz: bo),
        (mo_at, lambda zz: mo),
        (gu_at, lambda zz: gu.at[zz]),
        (dn_at, lambda zz: dn.at[zz]),
    )
    tok_copy = hop(tok, whole_tok.at[:, span(tp, half)], tok_sems.at[0], tok_sems.at[1], core_target)
    tok_copy.start()
    own = [pltpu.make_async_copy(tok, whole_tok.at[:, span(tp, half)], local.at[len(arrays)])]
    for a, (at, source) in enumerate(arrays):
        own.append(pltpu.make_async_copy(source(z), at(fs), local.at[a]))
    for copy in own:
        copy.start()

    line = {}
    for a, (at, source) in enumerate(arrays):
        for s in range(1, layers):
            line[a, s] = hop(
                source((z + s) % layers), at(fs), send.at[a, 0, s], recv.at[a, 0, s], on_line[s - 1]
            )
            line[a, s].start()

    sides, corners = {}, {}

    def start_sides(a, s):
        at, source = arrays[a]
        f = ((z - s + layers) % layers) * PLANE + p
        block = source(z) if s == 0 else at(f)
        for kind, target in ((1, x_target), (2, y_target)):
            sides[a, kind, s] = hop(block, at(f), send.at[a, kind, s], recv.at[a, kind, s], target)
            sides[a, kind, s].start()

    def start_corners(a, s):
        at, source = arrays[a]
        base = ((z - s + layers) % layers) * PLANE
        for kind, part, owner, target in ((1, 0, px, y_target), (2, 1, py, x_target)):
            sides[a, kind, s].wait_recv()
            block = at(base + owner, part)
            copy = hop(block, block, send.at[a, kind + 2, s], recv.at[a, kind + 2, s], target)
            copy.start()
            corners[a, kind, s] = copy

    steps = [(a, 0) for a in range(len(arrays))]
    for first in (0, 2):
        for s in range(1, layers):
            for a in (first, first + 1):
                steps.append((a, s))
    order = [(0, 0), (1, 0)] + [q for q in steps if q[0] < 2 and q[1] > 0]
    order += [(2, 0), (3, 0)] + [q for q in steps if q[0] > 1 and q[1] > 0]
    lag = 2
    for i in range(len(order) + lag):
        if i < len(order):
            a, s = order[i]
            if s > 0:
                line[a, s].wait_recv()
            start_sides(a, s)
        if i >= lag:
            start_corners(*order[i - lag])

    for a, s in order:
        if s > 0:
            line[a, s].wait_send()
        for kind in (1, 2):
            sides[a, kind, s].wait_send()
            corners[a, kind, s].wait()
    for copy in own:
        copy.wait()
    tok_copy.wait()


def gather_weights(layers, tok, bo, mo, gu, dn):
    n_fs = layers * PLANE
    shape = jax.ShapeDtypeStruct
    kind = jnp.bfloat16
    return pl.pallas_call(
        functools.partial(weights_kernel, layers),
        out_shape=(
            shape((tok.shape[0], 2 * tok.shape[1]), kind),
            shape((n_fs * bo.shape[0], bo.shape[1]), kind),
            shape((mo.shape[0], n_fs * mo.shape[1]), kind),
            shape((n_fs * gu.shape[1], gu.shape[2]), kind),
            shape((dn.shape[1], n_fs * dn.shape[2]), kind),
        ),
        in_specs=[ANY] * 5,
        out_specs=(ANY,) * 5,
        scratch_shapes=[
            pltpu.SemaphoreType.DMA((4, 5, layers)),
            pltpu.SemaphoreType.DMA((4, 5, layers)),
            pltpu.SemaphoreType.DMA((2,)),
            pltpu.SemaphoreType.DMA((5,)),
        ],
        compiler_params=pltpu.CompilerParams(collective_id=0, has_side_effects=True),
        name="gather_weights",
    )(tok, bo, mo, gu, dn)


def swap_kernel(mine, theirs, sems):
    target = (lax.axis_index("fs"), 1 - lax.axis_index("tp"))
    greet([target])
    copy = hop(mine, theirs, sems.at[0], sems.at[1], target)
    copy.start()
    copy.wait()


def swap_cores(values, number):
    return pl.pallas_call(
        swap_kernel,
        out_shape=jax.ShapeDtypeStruct(values.shape, values.dtype),
        in_specs=[ANY],
        out_specs=ANY,
        scratch_shapes=[pltpu.SemaphoreType.DMA((2,))],
        compiler_params=pltpu.CompilerParams(collective_id=number, has_side_effects=True),
        name="swap_cores",
    )(values)


def rows_kernel(layers, mine, whole, send, recv, local):
    fs, z, p, tp = where_am_i(layers)
    core_target = (fs, 1 - tp)
    on_line = line_targets(layers, z, p, tp)
    greet(on_line + [core_target])
    rows, half = mine.shape[0], mine.shape[1] // 2
    own = pltpu.make_async_copy(mine, whole.at[span(z, rows), :], local.at[0])
    line = {}
    for s in range(1, layers):
        line[s] = hop(
            mine.at[:, span(tp, half)],
            whole.at[span(z, rows), span(tp, half)],
            send.at[0, s],
            recv.at[0, s],
            on_line[s - 1],
        )
        line[s].start()
    own.start()
    across = {}
    for s in range(1, layers):
        line[s].wait_recv()
        block = whole.at[span((z - s + layers) % layers, rows), span(tp, half)]
        across[s] = hop(block, block, send.at[1, s], recv.at[1, s], core_target)
        across[s].start()
    for s in range(1, layers):
        line[s].wait_send()
        across[s].wait()
    own.wait()


def gather_rows(layers, values):
    return pl.pallas_call(
        functools.partial(rows_kernel, layers),
        out_shape=jax.ShapeDtypeStruct((layers * values.shape[0], values.shape[1]), values.dtype),
        in_specs=[ANY],
        out_specs=ANY,
        scratch_shapes=[
            pltpu.SemaphoreType.DMA((2, layers)),
            pltpu.SemaphoreType.DMA((2, layers)),
            pltpu.SemaphoreType.DMA((1,)),
        ],
        compiler_params=pltpu.CompilerParams(collective_id=2, has_side_effects=True),
        name="gather_rows",
    )(values)


def deal_kernel(layers, mine, dealt, send, recv):
    fs, z, p, tp = where_am_i(layers)
    on_line = line_targets(layers, z, p, tp)
    greet(on_line)
    line = {}
    for s in range(1, layers):
        line[s] = hop(
            mine.at[(z + s) % layers], dealt.at[s - 1], send.at[s], recv.at[s], on_line[s - 1]
        )
        line[s].start()
    for s in range(1, layers):
        line[s].wait()


def deal_rows(layers, values):
    return pl.pallas_call(
        functools.partial(deal_kernel, layers),
        out_shape=jax.ShapeDtypeStruct((layers - 1,) + values.shape[1:], values.dtype),
        in_specs=[ANY],
        out_specs=ANY,
        scratch_shapes=[
            pltpu.SemaphoreType.DMA((layers,)),
            pltpu.SemaphoreType.DMA((layers,)),
        ],
        compiler_params=pltpu.CompilerParams(collective_id=3, has_side_effects=True),
        name="deal_rows",
    )(values)


def split_layer(
    layers,
    tokens,
    mixer_norm_gain,
    recurrence_branch_weight,
    output_gate_projection,
    recurrence_conv_taps,
    recurrence_gate_map,
    input_gate_map,
    channel_decay_rate,
    position_log_decay,
    mixer_output_weight,
    feedforward_norm_gain,
    gate_up_weight,
    value_up_weight,
    gate_conv_taps,
    value_conv_taps,
    down_projection_weight,
):
    row_count, half = tokens.shape
    local_width = recurrence_branch_weight.shape[1]
    local_heads, head_size = recurrence_gate_map.shape[:2]
    deep, local_units = gate_up_weight.shape
    units = local_units // layers
    z, tp = lax.axis_index("fs") // PLANE, lax.axis_index("tp")
    bo = jnp.concatenate([recurrence_branch_weight, output_gate_projection], axis=1)
    gu = jnp.concatenate(
        [
            gate_up_weight.reshape(deep, layers, units),
            value_up_weight.reshape(deep, layers, units),
        ],
        axis=2,
    ).transpose(1, 0, 2)
    dn = down_projection_weight.reshape(layers, units, down_projection_weight.shape[1])
    whole_rows, bo_all, mo_all, gu_all, dn_all = gather_weights(
        layers, tokens, bo, mixer_output_weight, gu, dn
    )
    normed = rms_normed(whole_rows, mixer_norm_gain)
    both = jnp.dot(normed, bo_all, preferred_element_type=jnp.float32).astype(jnp.bfloat16)
    branch, outgate = both[:, :local_width], both[:, local_width:]
    conv = causal_conv(branch, recurrence_conv_taps).astype(jnp.bfloat16)
    grouped = conv.reshape(row_count, local_heads, head_size)

    def gate_of(weight):
        return jax.nn.sigmoid(
            jnp.einsum(
                "rhi,hij->rhj", grouped, weight, preferred_element_type=jnp.float32
            ).reshape(row_count, local_width)
        )

    recur, inner = gate_of(recurrence_gate_map), gate_of(input_gate_map)
    log_alpha = -DECAY_RATE_GAIN * recur * channel_decay_rate[None, :] + position_log_decay
    drive = jnp.sqrt(-jnp.expm1(2.0 * log_alpha)) * inner * conv.astype(jnp.float32)
    shape3 = (row_count // SEQ_LEN, SEQ_LEN, local_width)
    unused, state = lax.associative_scan(
        combine, (jnp.exp(log_alpha).reshape(shape3), drive.reshape(shape3)), axis=1
    )
    state = state.reshape(row_count, local_width)
    mixed = (state * jax.nn.gelu(outgate.astype(jnp.float32))).astype(jnp.bfloat16)
    mine = jnp.dot(mixed, mo_all, preferred_element_type=jnp.float32).astype(jnp.bfloat16)
    theirs = swap_cores(mine, 1)
    mixer_whole = mine.astype(jnp.float32) + theirs.astype(jnp.float32)
    whole_after = (whole_rows.astype(jnp.float32) + mixer_whole).astype(jnp.bfloat16)
    normed2 = gather_rows(layers, rms_normed(whole_after, feedforward_norm_gain))
    halves = jnp.dot(normed2, gu_all, preferred_element_type=jnp.float32).astype(jnp.bfloat16)
    gate_taps = lax.dynamic_slice_in_dim(gate_conv_taps, z * units, units, 1)
    value_taps = lax.dynamic_slice_in_dim(value_conv_taps, z * units, units, 1)
    hidden = (
        jax.nn.silu(causal_conv(halves[:, :units], gate_taps))
        * causal_conv(halves[:, units:], value_taps)
    ).astype(jnp.bfloat16)
    share = jnp.dot(hidden, dn_all, preferred_element_type=jnp.float32).astype(jnp.bfloat16)
    kept = lax.dynamic_slice_in_dim(share, tp * half, half, 1)
    given = lax.dynamic_slice_in_dim(share, (1 - tp) * half, half, 1)
    from_core = swap_cores(given, 4)
    paired = (kept.astype(jnp.float32) + from_core.astype(jnp.float32)).astype(jnp.bfloat16)
    paired = paired.reshape(layers, row_count, half)
    dealt = deal_rows(layers, paired)
    total = lax.dynamic_index_in_dim(paired, z, 0, keepdims=False).astype(jnp.float32)
    for s in range(layers - 1):
        total = total + dealt[s].astype(jnp.float32)
    residual = lax.dynamic_slice_in_dim(whole_after, tp * half, half, 1)
    return (residual.astype(jnp.float32) + total).astype(jnp.bfloat16)


def solution(mesh):
    placed = (
        P("fs", "tp"),
        P(),
        P("fs", "tp"),
        P("fs", "tp"),
        P(None, "tp"),
        P("tp", None, None),
        P("tp", None, None),
        P("tp"),
        P("fs", "tp"),
        P("tp", "fs"),
        P(),
        P("fs", "tp"),
        P("fs", "tp"),
        P(None, "tp"),
        P(None, "tp"),
        P("tp", "fs"),
    )
    n_fs, n_tp = mesh.shape["fs"], mesh.shape["tp"]
    layers = n_fs // PLANE
    body = gathered_layer
    if n_tp == 2 and n_fs % PLANE == 0 and layers > 1:
        body = functools.partial(split_layer, layers)
    return jax.shard_map(
        body, mesh=mesh, in_specs=placed, out_specs=P("fs", "tp"), check_vma=False
    )
```

```python
import functools

import jax
import jax.numpy as jnp
from jax import lax
from jax.experimental import pallas as pl
from jax.experimental.pallas import tpu as pltpu
from jax.sharding import PartitionSpec as P

SEQ_LEN = 64


EPS = 1e-06
DECAY_RATE_GAIN = 8.0


def rms_normed(values, gain):
    wide = values.astype(jnp.float32)
    factor = lax.rsqrt(jnp.mean(wide * wide, axis=-1, keepdims=True) + EPS)
    return (wide * factor * gain.astype(jnp.float32)).astype(jnp.bfloat16)


def causal_conv(values, kernel):
    width = kernel.shape[0]
    row_count, channels = values.shape
    grouped = values.astype(jnp.float32).reshape(row_count // SEQ_LEN, SEQ_LEN, channels)
    padded = jnp.pad(grouped, ((0, 0), (width - 1, 0), (0, 0)))
    summed = padded[:, 0:SEQ_LEN] * kernel[0].astype(jnp.float32)
    for offset in range(1, width):
        summed = summed + padded[:, offset : offset + SEQ_LEN] * kernel[offset].astype(jnp.float32)
    return summed.reshape(row_count, channels)


def combine(left, right):
    first_a, first_b = left
    second_a, second_b = right
    return (first_a * second_a, second_a * first_b + second_b)


def pair_folder(normed, pieces):
    return (
        jnp.dot(normed, pieces[0], preferred_element_type=jnp.float32),
        jnp.dot(normed, pieces[1], preferred_element_type=jnp.float32),
    )


def gathered_layer(
    tokens,
    mixer_norm_gain,
    recurrence_branch_weight,
    output_gate_projection,
    recurrence_conv_taps,
    recurrence_gate_map,
    input_gate_map,
    channel_decay_rate,
    position_log_decay,
    mixer_output_weight,
    feedforward_norm_gain,
    gate_up_weight,
    value_up_weight,
    gate_conv_taps,
    value_conv_taps,
    down_projection_weight,
):
    row_count = tokens.shape[0]
    local_width = recurrence_branch_weight.shape[1]
    local_heads = recurrence_gate_map.shape[0]
    head_size = recurrence_gate_map.shape[1]
    whole_rows = lax.all_gather(tokens, "tp", axis=1, tiled=True)
    normed = rms_normed(whole_rows, mixer_norm_gain)
    branch_sum, outgate_sum = pair_folder(
        normed,
        (
            lax.all_gather(recurrence_branch_weight, "fs", axis=0, tiled=True),
            lax.all_gather(output_gate_projection, "fs", axis=0, tiled=True),
        ),
    )
    branch = branch_sum.astype(jnp.bfloat16)
    outgate = outgate_sum.astype(jnp.bfloat16)
    conv = causal_conv(branch, recurrence_conv_taps).astype(jnp.bfloat16)
    grouped = conv.reshape(row_count, local_heads, head_size)
    recurrence_scan = jax.nn.sigmoid(
        jnp.einsum(
            "rhi,hij->rhj", grouped, recurrence_gate_map, preferred_element_type=jnp.float32
        ).reshape(row_count, local_width)
    )
    inner = jax.nn.sigmoid(
        jnp.einsum(
            "rhi,hij->rhj", grouped, input_gate_map, preferred_element_type=jnp.float32
        ).reshape(row_count, local_width)
    )
    log_alpha = (
        -DECAY_RATE_GAIN * recurrence_scan * channel_decay_rate[None, :] + position_log_decay
    )
    drive = jnp.sqrt(-jnp.expm1(2.0 * log_alpha)) * inner * conv.astype(jnp.float32)
    shape3 = (row_count // SEQ_LEN, SEQ_LEN, local_width)
    _, state = lax.associative_scan(
        combine, (jnp.exp(log_alpha).reshape(shape3), drive.reshape(shape3)), axis=1
    )
    state = state.reshape(row_count, local_width)
    mixed = (state * jax.nn.gelu(outgate.astype(jnp.float32))).astype(jnp.bfloat16)
    mixer_terms = jnp.dot(
        mixed,
        lax.all_gather(mixer_output_weight, "fs", axis=1, tiled=True),
        preferred_element_type=jnp.float32,
    )
    mixer_terms = mixer_terms.astype(jnp.bfloat16).astype(jnp.float32)
    mixer_whole = lax.psum(mixer_terms.astype(jnp.bfloat16), "tp").astype(jnp.float32)
    whole_after = (whole_rows.astype(jnp.float32) + mixer_whole).astype(jnp.bfloat16)
    normed2 = rms_normed(whole_after, feedforward_norm_gain)
    gate_whole, value_whole = (
        lax.all_gather(gate_up_weight, "fs", axis=0, tiled=True),
        lax.all_gather(value_up_weight, "fs", axis=0, tiled=True),
    )
    gate_sum = jnp.dot(normed2, gate_whole, preferred_element_type=jnp.float32)
    value_sum = jnp.dot(normed2, value_whole, preferred_element_type=jnp.float32)
    gate_half = gate_sum.astype(jnp.bfloat16)
    value_half = value_sum.astype(jnp.bfloat16)
    hidden = (
        jax.nn.silu(causal_conv(gate_half, gate_conv_taps))
        * causal_conv(value_half, value_conv_taps)
    ).astype(jnp.bfloat16)
    channel_terms = jnp.dot(
        hidden,
        lax.all_gather(down_projection_weight, "fs", axis=1, tiled=True),
        preferred_element_type=jnp.float32,
    )
    channel_terms = channel_terms.astype(jnp.bfloat16).astype(jnp.float32)
    channel_share = lax.psum_scatter(
        channel_terms.astype(jnp.bfloat16), "tp", scatter_dimension=1, tiled=True
    ).astype(jnp.float32)
    share_width = channel_share.shape[1]
    residual_share = lax.dynamic_slice_in_dim(
        whole_after, lax.axis_index("tp") * share_width, share_width, 1
    )
    return (residual_share.astype(jnp.float32) + channel_share).astype(jnp.bfloat16)


PLANE = 4
ANY = pl.BlockSpec(memory_space=pl.ANY)


def hop(src, dst, send, recv, target):
    return pltpu.make_async_remote_copy(
        src_ref=src,
        dst_ref=dst,
        send_sem=send,
        recv_sem=recv,
        device_id=target,
        device_id_type=pl.DeviceIdType.MESH,
    )


def greet(targets):
    barrier = pltpu.get_barrier_semaphore()
    for target in targets:
        pl.semaphore_signal(
            barrier, inc=1, device_id=target, device_id_type=pl.DeviceIdType.MESH
        )
    pl.semaphore_wait(barrier, len(targets))


def span(index, size):
    return pl.ds(pl.multiple_of(index * size, size), size)


def where_am_i():
    fs, tp = lax.axis_index("fs"), lax.axis_index("tp")
    return fs, fs // PLANE, fs % PLANE, tp


def line_targets(layers, z, p, tp):
    return [(((z + s) % layers) * PLANE + p, tp) for s in range(1, layers)]


def share_plane(layers, z, p, tp, arrays, order, send, recv, arrived):
    y, x = p // 2, p % 2
    px, py = y * 2 + (x + 1) % 2, ((y + 1) % 2) * 2 + x
    x_target, y_target = (z * PLANE + px, tp), (z * PLANE + py, tp)
    sides, corners = {}, {}

    def start_sides(a, s):
        at, source = arrays[a]
        f = ((z - s + layers) % layers) * PLANE + p
        block = source(z) if s == 0 else at(f)
        for kind, target in ((1, x_target), (2, y_target)):
            sides[a, kind, s] = hop(block, at(f), send.at[a, kind, s], recv.at[a, kind, s], target)
            sides[a, kind, s].start()

    def start_corners(a, s):
        at, _ = arrays[a]
        base = ((z - s + layers) % layers) * PLANE
        for kind, part, owner, target in ((1, 0, px, y_target), (2, 1, py, x_target)):
            sides[a, kind, s].wait_recv()
            block = at(base + owner, part)
            copy = hop(block, block, send.at[a, kind + 2, s], recv.at[a, kind + 2, s], target)
            copy.start()
            corners[a, kind, s] = copy

    lag = 2
    for i in range(len(order) + lag):
        if i < len(order):
            arrived(*order[i])
            start_sides(*order[i])
        if i >= lag:
            start_corners(*order[i - lag])

    def finish():
        for copy in sides.values():
            copy.wait_send()
        for copy in corners.values():
            copy.wait()

    return finish


def row_blocks(whole, deep):
    def at(f, part=None):
        if part is None:
            return whole.at[span(f, deep), :]
        return whole.at[span(f * 2 + part, deep // 2), :]

    return at


def column_blocks(whole, wide):
    rows = whole.shape[0]

    def at(f, part=None):
        if part is None:
            return whole.at[:, span(f, wide)]
        return whole.at[pl.ds(part * (rows // 2), rows // 2), span(f, wide)]

    return at


def plane_targets(z, p, tp):
    y, x = p // 2, p % 2
    px, py = y * 2 + (x + 1) % 2, ((y + 1) % 2) * 2 + x
    return [(z * PLANE + px, tp), (z * PLANE + py, tp)]


def weights_kernel(
    layers, tok, bo, mo, gu, dn, whole_tok, bo_all, mo_all, gu_all, dn_all, send, recv, tok_sems, local
):
    fs, z, p, tp = where_am_i()
    core_target = (fs, 1 - tp)
    on_line = line_targets(layers, z, p, tp)
    greet(on_line + plane_targets(z, p, tp) + [core_target])

    half = tok.shape[1]
    deep = bo.shape[0]
    wide = mo.shape[1]

    arrays = (
        (row_blocks(bo_all, deep), lambda zz: bo),
        (column_blocks(mo_all, wide), lambda zz: mo),
        (row_blocks(gu_all, deep), lambda zz: gu.at[zz]),
        (column_blocks(dn_all, wide), lambda zz: dn.at[zz]),
    )
    tok_copy = hop(tok, whole_tok.at[:, span(tp, half)], tok_sems.at[0], tok_sems.at[1], core_target)
    tok_copy.start()
    own = [pltpu.make_async_copy(tok, whole_tok.at[:, span(tp, half)], local.at[len(arrays)])]
    for a, (at, source) in enumerate(arrays):
        own.append(pltpu.make_async_copy(source(z), at(fs), local.at[a]))
    for copy in own:
        copy.start()

    line = {}
    for a, (at, source) in enumerate(arrays):
        for s in range(1, layers):
            line[a, s] = hop(
                source((z + s) % layers), at(fs), send.at[a, 0, s], recv.at[a, 0, s], on_line[s - 1]
            )
            line[a, s].start()

    def arrived(a, s):
        if s > 0:
            line[a, s].wait_recv()

    order = [(a, 0) for a in range(2)]
    order += [(a, s) for s in range(1, layers) for a in range(2)]
    order += [(2, s) for s in range(layers // 2)]
    finish = share_plane(layers, z, p, tp, arrays, order, send, recv, arrived)
    for a, s in line:
        if (a, s) not in order:
            line[a, s].wait_recv()
    finish()
    for copy in line.values():
        copy.wait_send()
    for copy in own:
        copy.wait()
    tok_copy.wait()


def gather_weights(layers, tok, bo, mo, gu, dn):
    n_fs = layers * PLANE
    shape = jax.ShapeDtypeStruct
    kind = jnp.bfloat16
    return pl.pallas_call(
        functools.partial(weights_kernel, layers),
        out_shape=(
            shape((tok.shape[0], 2 * tok.shape[1]), kind),
            shape((n_fs * bo.shape[0], bo.shape[1]), kind),
            shape((mo.shape[0], n_fs * mo.shape[1]), kind),
            shape((n_fs * gu.shape[1], gu.shape[2]), kind),
            shape((dn.shape[1], n_fs * dn.shape[2]), kind),
        ),
        in_specs=[ANY] * 5,
        out_specs=(ANY,) * 5,
        scratch_shapes=[
            pltpu.SemaphoreType.DMA((4, 5, layers)),
            pltpu.SemaphoreType.DMA((4, 5, layers)),
            pltpu.SemaphoreType.DMA((2,)),
            pltpu.SemaphoreType.DMA((5,)),
        ],
        compiler_params=pltpu.CompilerParams(collective_id=0, has_side_effects=True),
        name="gather_weights",
    )(tok, bo, mo, gu, dn)


def swap_kernel(mine, theirs, sems):
    target = (lax.axis_index("fs"), 1 - lax.axis_index("tp"))
    greet([target])
    copy = hop(mine, theirs, sems.at[0], sems.at[1], target)
    copy.start()
    copy.wait()


def swap_cores(values, number):
    return pl.pallas_call(
        swap_kernel,
        out_shape=jax.ShapeDtypeStruct(values.shape, values.dtype),
        in_specs=[ANY],
        out_specs=ANY,
        scratch_shapes=[pltpu.SemaphoreType.DMA((2,))],
        compiler_params=pltpu.CompilerParams(collective_id=number, has_side_effects=True),
        name="swap_cores",
    )(values)


def rows_kernel(
    layers, mine, gu_in, dn_in, whole, gu_all, dn_all, send, recv, plane_send, plane_recv, local
):
    fs, z, p, tp = where_am_i()
    core_target = (fs, 1 - tp)
    on_line = line_targets(layers, z, p, tp)
    greet(on_line + plane_targets(z, p, tp) + [core_target])
    rows, half = mine.shape[0], mine.shape[1] // 2
    own = pltpu.make_async_copy(mine, whole.at[pl.ds((layers - 1) * rows, rows), :], local.at[0])
    line, across = {}, {}
    for s in range(1, layers):
        line[s] = hop(
            mine.at[:, span(tp, half)],
            whole.at[pl.ds((layers - 1 - s) * rows, rows), span(tp, half)],
            send.at[0, s],
            recv.at[0, s],
            on_line[s - 1],
        )
        line[s].start()
    own.start()
    n_fs = layers * PLANE
    arrays = []
    for at in (row_blocks(gu_all, gu_all.shape[0] // n_fs), column_blocks(dn_all, dn_all.shape[1] // n_fs)):
        arrays.append((at, lambda zz, at=at: at(zz * PLANE + p)))
    order = [(0, s) for s in range(layers // 2, layers)] + [(1, s) for s in range(layers)]
    finish = share_plane(
        layers, z, p, tp, arrays, order, plane_send, plane_recv, lambda a, s: None
    )
    for s in range(1, layers):
        line[s].wait_recv()
        block = whole.at[pl.ds((layers - 1 - s) * rows, rows), span(tp, half)]
        across[s] = hop(block, block, send.at[1, s], recv.at[1, s], core_target)
        across[s].start()
    for s in range(1, layers):
        line[s].wait_send()
        across[s].wait()
    finish()
    own.wait()


def gather_rows(layers, values, gu_all, dn_all):
    whole = jax.ShapeDtypeStruct((layers * values.shape[0], values.shape[1]), values.dtype)
    return pl.pallas_call(
        functools.partial(rows_kernel, layers),
        out_shape=(
            whole,
            jax.ShapeDtypeStruct(gu_all.shape, gu_all.dtype),
            jax.ShapeDtypeStruct(dn_all.shape, dn_all.dtype),
        ),
        in_specs=[ANY] * 3,
        out_specs=(ANY,) * 3,
        input_output_aliases={1: 1, 2: 2},
        scratch_shapes=[
            pltpu.SemaphoreType.DMA((2, layers)),
            pltpu.SemaphoreType.DMA((2, layers)),
            pltpu.SemaphoreType.DMA((2, 5, layers)),
            pltpu.SemaphoreType.DMA((2, 5, layers)),
            pltpu.SemaphoreType.DMA((1,)),
        ],
        compiler_params=pltpu.CompilerParams(collective_id=2, has_side_effects=True),
        name="gather_rows",
    )(values, gu_all, dn_all)


def swap_half_kernel(mine, theirs, sems):
    tp = lax.axis_index("tp")
    target = (lax.axis_index("fs"), 1 - tp)
    greet([target])
    copy = hop(mine.at[:, span(1 - tp, theirs.shape[1])], theirs, sems.at[0], sems.at[1], target)
    copy.start()
    copy.wait()


def swap_halves(values, number):
    return pl.pallas_call(
        swap_half_kernel,
        out_shape=jax.ShapeDtypeStruct((values.shape[0], values.shape[1] // 2), values.dtype),
        in_specs=[ANY],
        out_specs=ANY,
        scratch_shapes=[pltpu.SemaphoreType.DMA((2,))],
        compiler_params=pltpu.CompilerParams(collective_id=number, has_side_effects=True),
        name="swap_halves",
    )(values)


def split_layer(
    layers,
    tokens,
    mixer_norm_gain,
    recurrence_branch_weight,
    output_gate_projection,
    recurrence_conv_taps,
    recurrence_gate_map,
    input_gate_map,
    channel_decay_rate,
    position_log_decay,
    mixer_output_weight,
    feedforward_norm_gain,
    gate_up_weight,
    value_up_weight,
    gate_conv_taps,
    value_conv_taps,
    down_projection_weight,
):
    row_count, half = tokens.shape
    local_width = recurrence_branch_weight.shape[1]
    local_heads, head_size = recurrence_gate_map.shape[:2]
    deep, local_units = gate_up_weight.shape
    units = local_units // layers
    z, tp = lax.axis_index("fs") // PLANE, lax.axis_index("tp")
    bo = jnp.concatenate([recurrence_branch_weight, output_gate_projection], axis=1)
    gu = jnp.concatenate(
        [
            gate_up_weight.reshape(deep, layers, units),
            value_up_weight.reshape(deep, layers, units),
        ],
        axis=2,
    ).transpose(1, 0, 2)
    dn = down_projection_weight.reshape(layers, units, down_projection_weight.shape[1])
    whole_rows, bo_all, mo_all, gu_all, dn_all = gather_weights(
        layers, tokens, bo, mixer_output_weight, gu, dn
    )
    normed = rms_normed(whole_rows, mixer_norm_gain)
    both = jnp.dot(normed, bo_all, preferred_element_type=jnp.float32).astype(jnp.bfloat16)
    branch, outgate = both[:, :local_width], both[:, local_width:]
    conv = causal_conv(branch, recurrence_conv_taps).astype(jnp.bfloat16)
    grouped = conv.reshape(row_count, local_heads, head_size)

    def gate_of(weight):
        return jax.nn.sigmoid(
            jnp.einsum(
                "rhi,hij->rhj", grouped, weight, preferred_element_type=jnp.float32
            ).reshape(row_count, local_width)
        )

    recur, inner = gate_of(recurrence_gate_map), gate_of(input_gate_map)
    log_alpha = -DECAY_RATE_GAIN * recur * channel_decay_rate[None, :] + position_log_decay
    drive = jnp.sqrt(-jnp.expm1(2.0 * log_alpha)) * inner * conv.astype(jnp.float32)
    shape3 = (row_count // SEQ_LEN, SEQ_LEN, local_width)
    _, state = lax.associative_scan(
        combine, (jnp.exp(log_alpha).reshape(shape3), drive.reshape(shape3)), axis=1
    )
    state = state.reshape(row_count, local_width)
    mixed = (state * jax.nn.gelu(outgate.astype(jnp.float32))).astype(jnp.bfloat16)
    mine = jnp.dot(mixed, mo_all, preferred_element_type=jnp.float32).astype(jnp.bfloat16)
    theirs = swap_cores(mine, 1)
    mixer_whole = mine.astype(jnp.float32) + theirs.astype(jnp.float32)
    whole_after = (whole_rows.astype(jnp.float32) + mixer_whole).astype(jnp.bfloat16)
    normed2, gu_all, dn_all = gather_rows(
        layers, rms_normed(whole_after, feedforward_norm_gain), gu_all, dn_all
    )
    gate_taps = lax.dynamic_slice_in_dim(gate_conv_taps, z * units, units, 1)
    value_taps = lax.dynamic_slice_in_dim(value_conv_taps, z * units, units, 1)
    n_fs = layers * PLANE

    def share_of(rows, number):
        halves = jnp.dot(rows, gu_all, preferred_element_type=jnp.float32)
        halves = halves.astype(jnp.bfloat16)
        hidden = (
            jax.nn.silu(causal_conv(halves[:, :units], gate_taps))
            * causal_conv(halves[:, units:], value_taps)
        ).astype(jnp.bfloat16)
        share = jnp.dot(hidden, dn_all, preferred_element_type=jnp.float32).astype(jnp.bfloat16)
        kept = lax.dynamic_slice_in_dim(share, tp * half, half, 1)
        paired = kept.astype(jnp.float32) + swap_halves(share, number).astype(jnp.float32)
        return paired.astype(jnp.bfloat16)

    def deal(paired, first):
        sent = []
        for i in range(paired.shape[0] // row_count):
            s = first + i
            block = paired[i * row_count : (i + 1) * row_count]
            if s == layers:
                sent.append(block)
            else:
                route = [(f, (f + s * PLANE) % n_fs) for f in range(n_fs)]
                sent.append(lax.ppermute(block, "fs", route))
        return sent

    cut = layers // 2
    early_rows, late_rows = normed2[: cut * row_count], normed2[cut * row_count :]
    early = share_of(early_rows, 4)
    late_rows, early = lax.optimization_barrier((late_rows, early))
    dealt = deal(early, 1)
    late = share_of(late_rows, 5)
    dealt += deal(late, cut + 1)
    total = dealt[-1].astype(jnp.float32)
    for term in dealt[:-1]:
        total = total + term.astype(jnp.float32)
    residual = lax.dynamic_slice_in_dim(whole_after, tp * half, half, 1)
    return (residual.astype(jnp.float32) + total).astype(jnp.bfloat16)


def solution(mesh):
    placed = (
        P("fs", "tp"),
        P(),
        P("fs", "tp"),
        P("fs", "tp"),
        P(None, "tp"),
        P("tp", None, None),
        P("tp", None, None),
        P("tp"),
        P("fs", "tp"),
        P("tp", "fs"),
        P(),
        P("fs", "tp"),
        P("fs", "tp"),
        P(None, "tp"),
        P(None, "tp"),
        P("tp", "fs"),
    )
    n_fs, n_tp = mesh.shape["fs"], mesh.shape["tp"]
    layers = n_fs // PLANE
    body = gathered_layer
    if n_tp == 2 and n_fs % PLANE == 0 and layers > 1:
        body = functools.partial(split_layer, layers)
    return jax.shard_map(
        body, mesh=mesh, in_specs=placed, out_specs=P("fs", "tp"), check_vma=False
    )
```
